32 devices in a mesh: sp: 8 (over z, y), tp: 4 (over x, core).
Axes of the slice: x: 2, y: 2, z: 4, core: 2. Of those that a mesh axis runs over, the one named last changes fastest.
Arguments:
- normalized_sequence: bfloat16 [2048, 3072], P('sp', 'tp'), may hold values from -6 to 6
- probe_projection: bfloat16 [3072, 1024], P(None, 'tp'), may hold values from -0.109375 to 0.109375
- payload_array: bfloat16 [2048, 1024], P('sp', 'tp'), may hold values from -6 to 6
- onward_retain_scores: bfloat16 [2048, 1024], P('sp', 'tp'), may hold values from -5 to 5
- reverse_retain_scores: bfloat16 [2048, 1024], P('sp', 'tp'), may hold values from -5 to 5
- retention_slack: float32 [2, 1024], P(None, 'tp'), as said below
- additional_decay: float32 [2, 2048, 8], P(None, 'sp', 'tp'), may hold values from -1.38 to 0, as said below
- rescale_weights: float32 [1024], P('tp'), may hold values from 0.1 to 1.9
- result_cotangent: bfloat16 [2048, 1024], P('sp', 'tp'), may hold values from -6 to 6
Outputs:
- query_pre_grad: bfloat16 [2048, 1024], P('sp', 'tp')
- gate_fwd_grad: float32 [2048, 1024], P('sp', 'tp')
- gate_bwd_grad: float32 [2048, 1024], P('sp', 'tp')
- value_grad: bfloat16 [2048, 1024], P('sp', 'tp')
- query_weight_grad: float32 [3072, 1024], P('sp', 'tp')
The draws below stay inside these ranges and needn't reach their ends.
Inputs may be any that keep to these rules, and one draw needn't show every extreme that they name: `retention_slack`: every entry is positive. `additional_decay`: zero except at a few positions.
All inputs are finite; a program needn't handle non-finite values.
Results may differ from the reference program's by a relative error of at most 0.025.
Values may be sent and summed in bfloat16 or wider, within the bound.
A program may use at most 64 MiB of HBM per device.

```python
import math
import jax
import jax.numpy as jnp
from jax import lax

D = 3072
HEADS = 8
ATTENTION_WIDTH = 128
BLOCK = 128
TOK_DEV = 256
TOKENS = 2048
HW = 1024


def draw_retention_slack(key, part):
    chooser, slow_key, fast_key = jax.random.split(key, 3)
    fast_share = 0.5
    fast_heads = jax.random.bernoulli(chooser, fast_share, (2, HEADS, 1))
    slow_gap = jnp.exp(jax.random.uniform(slow_key, (2, HEADS, ATTENTION_WIDTH), jnp.float32, math.log(0.3), math.log(1.5))) / TOKENS
    fast_gap = jnp.exp(jax.random.uniform(fast_key, (2, HEADS, ATTENTION_WIDTH), jnp.float32, math.log(0.02), math.log(0.06)))
    return jnp.where(fast_heads, fast_gap, slow_gap).reshape(2, HEADS * ATTENTION_WIDTH)


def draw_additional_decay(key, part):
    place_key, depth_key = jax.random.split(key)
    spike_places = jax.random.randint(place_key, (2, 2, HEADS), 0, TOKENS)
    depth_levels = jax.random.uniform(depth_key, (2, 2, HEADS), jnp.float32, 0.22, 0.69)
    token_positions = jnp.arange(TOKENS)[None, :, None]
    total_output = jnp.zeros((2, TOKENS, HEADS), jnp.float32)
    for spike_index in range(2):
        spike_hits = token_positions == spike_places[:, spike_index][:, None, :]
        total_output = total_output - jnp.where(spike_hits, depth_levels[:, spike_index][:, None, :], 0.0)
    return total_output


def shifted_gates(key, salt):
    noise_key, shift_key = jax.random.split(jax.random.fold_in(key, salt))
    noise = jax.random.truncated_normal(noise_key, -4.0, 4.0, (TOKENS, HEADS * ATTENTION_WIDTH), jnp.float32)
    shifts = jax.random.uniform(shift_key, (TOKENS // TOK_DEV, 1, HEADS, 1), jnp.float32, -1.0, 1.0)
    shifted = noise.reshape(TOKENS // TOK_DEV, TOK_DEV, HEADS, ATTENTION_WIDTH) + shifts
    return shifted.reshape(TOKENS, HEADS * ATTENTION_WIDTH)


def draw_onward_retain_scores(key, part):
    return shifted_gates(key, 11).astype(jnp.bfloat16)


def draw_reverse_retain_scores(key, part):
    return shifted_gates(key, 12).astype(jnp.bfloat16)


def shard_levels(own_key, shape, pieces, low, largest):
    def one(dim, parts):
        draws = jax.random.uniform(jax.random.fold_in(jax.random.fold_in(own_key, 6), dim), (parts,), jnp.float32, low / len(pieces), largest / len(pieces))
        return jnp.repeat(jnp.exp(draws), shape[dim] // parts).reshape((-1,) + (1,) * (len(shape) - dim - 1))

    factor_of = one(*pieces[0])
    for cut in pieces[1:]:
        factor_of = factor_of * one(*cut)
    return factor_of


def bell_draw(key, shape, width, limit, shards=(), kind=jnp.bfloat16):
    result = jax.random.normal(key, shape, jnp.float32) * width
    if len(shards) > 0:
        result = shard_levels(key, shape, shards, -0.22, 0.18) * result
    return jnp.clip(result, min=-limit, max=limit).astype(kind)


def setup_inputs(seed: int = 0) -> dict:
    seeds = jax.random.split(jax.random.key(seed), 10)
    return {
        "normalized_sequence": bell_draw(seeds[0], (TOKENS, D), 1.0, 6.0, ((0, 8), (1, 4))),
        "probe_projection": bell_draw(seeds[1], (D, HW), D ** -0.5, 0.109375, ((1, 4),)),
        "payload_array": bell_draw(seeds[2], (TOKENS, HW), 1.0, 6.0, ((0, 8), (1, 4))),
        "onward_retain_scores": draw_onward_retain_scores(jax.random.fold_in(seeds[9], 71), 0),
        "reverse_retain_scores": draw_reverse_retain_scores(jax.random.fold_in(seeds[9], 71), 0),
        "retention_slack": draw_retention_slack(jax.random.fold_in(seeds[9], 71), 0),
        "additional_decay": draw_additional_decay(jax.random.fold_in(seeds[9], 71), 0),
        "rescale_weights": jnp.clip(1.0 + 0.18 * jax.random.normal(seeds[7], (HW,), jnp.float32), 0.1, 1.9),
        "result_cotangent": bell_draw(seeds[8], (TOKENS, HW), 1.0, 6.0, ((0, 8), (1, 4))),
    }


epsilon = 1e-06

def recurrence(queries, key_matrix, values, forget_logarithm, initial):
    length, attention_count = (queries.shape[0], queries.shape[1])
    block_count = length // BLOCK
    within_mask = jnp.tril(jnp.ones((BLOCK, BLOCK), bool))
    highest = lax.Precision.HIGHEST

    def advance(carried_state, segment):
        query_seg, key_seg, value_seg, forget_seg = segment
        running = jnp.cumsum(forget_seg, axis=0)
        query_dec = query_seg * jnp.exp(running)
        key_dec = key_seg * jnp.exp(-running)
        scores = jnp.einsum('thd,shd->hts', query_dec, key_dec, precision=highest)
        scores = jnp.where(within_mask[None], scores, 0.0)
        output = jnp.einsum('hts,she->the', scores, value_seg, precision=highest)
        output = output + jnp.einsum('thd,hde->the', query_dec, carried_state, precision=highest)
        closing = running[-1]
        carried_state = jnp.exp(closing)[:, :, None] * carried_state + jnp.einsum('shd,she->hde', key_seg * jnp.exp(closing[None] - running), value_seg, precision=highest)
        return (carried_state, output)
    blocks = tuple((member.reshape((block_count, BLOCK) + member.shape[1:]) for member in (queries, key_matrix, values, forget_logarithm)))
    final_state, outputs = lax.scan(jax.checkpoint(advance), initial, blocks)
    return outputs.reshape(length, attention_count, values.shape[2])

def retention_update(gate_input_rows, margin_row, spike_column):
    key_matrix = margin_row * jax.nn.sigmoid(-gate_input_rows)
    forget_logarithm = jnp.log1p(-key_matrix) + spike_column[:, :, None]
    return (key_matrix, forget_logarithm)

def blending_update(probe_before_activation, onward_raw_scores, reverse_raw_scores, payload_entries, onward_seed_memory, reverse_seed_memory, retention_slack, additional_decay, rescale_weights):
    length = probe_before_activation.shape[0]
    attention_count = probe_before_activation.shape[1] // ATTENTION_WIDTH

    def partition_attention(array):
        return array.reshape(length, attention_count, ATTENTION_WIDTH)
    queries = partition_attention(jax.nn.silu(probe_before_activation) * ATTENTION_WIDTH ** (-0.5))
    values = partition_attention(payload_entries)
    onward_addressing, onward_retention = retention_update(partition_attention(onward_raw_scores), retention_slack[0].reshape(attention_count, ATTENTION_WIDTH), additional_decay[0])
    reverse_addressing, reverse_retention = retention_update(partition_attention(reverse_raw_scores), retention_slack[1].reshape(attention_count, ATTENTION_WIDTH), additional_decay[1])
    out_fwd = recurrence(queries, onward_addressing, values, onward_retention, onward_seed_memory)
    out_bwd = jnp.flip(recurrence(jnp.flip(queries, 0), jnp.flip(reverse_addressing, 0), jnp.flip(values, 0), jnp.flip(reverse_retention, 0), reverse_seed_memory), 0)
    mixed = out_fwd + out_bwd
    normed = mixed * lax.rsqrt(lax.optimization_barrier(jnp.mean(mixed * mixed, axis=-1, keepdims=True)) + epsilon)
    normed = normed * rescale_weights.reshape(attention_count, ATTENTION_WIDTH)
    return normed.reshape(length, attention_count * ATTENTION_WIDTH)

def reference(normalized_sequence, probe_projection, payload_array, onward_retain_scores, reverse_retain_scores, retention_slack, additional_decay, rescale_weights, result_cotangent):
    probe_before_activation = jnp.dot(normalized_sequence, probe_projection, preferred_element_type=jnp.float32).astype(jnp.bfloat16)
    attention_count = probe_projection.shape[1] // ATTENTION_WIDTH
    blank_memory = jnp.zeros((attention_count, ATTENTION_WIDTH, ATTENTION_WIDTH), jnp.float32)

    def forward(probe_raw_scores, onward_raw_scores, reverse_raw_scores, payload_entries):
        return blending_update(probe_raw_scores, onward_raw_scores, reverse_raw_scores, payload_entries, blank_memory, blank_memory, retention_slack, additional_decay, rescale_weights)
    unused, pullback = jax.vjp(forward, probe_before_activation.astype(jnp.float32), onward_retain_scores.astype(jnp.float32), reverse_retain_scores.astype(jnp.float32), payload_array.astype(jnp.float32))
    grad_query, grad_fwd, grad_bwd, grad_value = pullback(result_cotangent.astype(jnp.float32))
    query_pre_grad = grad_query.astype(jnp.bfloat16)
    weight_grad = lax.dot_general(normalized_sequence, query_pre_grad, (((0,), (0,)), ((), ())), preferred_element_type=jnp.float32)
    return (query_pre_grad, grad_fwd, grad_bwd, grad_value.astype(jnp.bfloat16), weight_grad)
```

```python
import functools

import jax
import jax.numpy as jnp
from jax import lax
from jax.experimental import pallas as pl
from jax.experimental.pallas import tpu as pltpu
from jax.sharding import PartitionSpec as P

WIDTH = 128
EXTRA = 16
EPSILON = 1e-06
F32 = jnp.float32
BF16 = jnp.bfloat16


def dot(a, b, ca, cb):
    return lax.dot_general(a, b, (((ca,), (cb,)), ((), ())), preferred_element_type=F32)


def nn(a, b):
    return dot(a, b, 1, 0)


def nt(a, b):
    return dot(a, b, 1, 1)


def tn(a, b):
    return dot(a, b, 0, 0)


def split(a):
    hi = a.astype(BF16)
    return hi, (a - hi.astype(F32)).astype(BF16)


def split_dot(tri, a):
    hi, lo = split(a)
    return nn(tri, hi) + nn(tri, lo)


def sigmoid(x):
    return 1.0 / (1.0 + jnp.exp(-x))


def kernel(
    nsp,
    ntp,
    x_hbm,
    w_hbm,
    v_ref,
    f_ref,
    r_ref,
    slack_ref,
    decay_ref,
    gain_ref,
    cot_ref,
    dq_ref,
    gf_ref,
    gb_ref,
    dv_ref,
    wg_ref,
    xg,
    wv,
    msg1,
    got1,
    msg2,
    got2,
    acc,
    part,
    terms,
    run_s,
    dqs_s,
    loc_s,
    dk_s,
    local_sem,
    x_send,
    x_recv,
    a_send,
    a_recv,
    b_send,
    b_recv,
    c_send,
    c_recv,
):
    sp = lax.axis_index("sp")
    tp = lax.axis_index("tp")
    length, width = v_ref.shape
    heads = width // WIDTH
    feat = x_hbm.shape[1]
    rows = wg_ref.shape[0]
    half = length // 2

    own_x = pltpu.make_async_copy(x_hbm, xg.at[0], local_sem.at[0])
    own_w = pltpu.make_async_copy(w_hbm, wv, local_sem.at[1])
    own_x.start()
    own_w.start()

    barrier = pltpu.get_barrier_semaphore()

    @pl.loop(1, ntp)
    def _(o):
        pl.semaphore_signal(
            barrier, inc=1, device_id={"tp": lax.rem(tp + o, ntp)}, device_id_type=pl.DeviceIdType.MESH
        )

    @pl.loop(1, nsp)
    def _(o):
        pl.semaphore_signal(
            barrier, inc=1, device_id={"sp": lax.rem(sp + o, nsp)}, device_id_type=pl.DeviceIdType.MESH
        )

    pl.semaphore_wait(barrier, nsp + ntp - 2)

    def x_copy(o):
        return pltpu.make_async_remote_copy(
            src_ref=x_hbm,
            dst_ref=xg.at[o],
            send_sem=x_send.at[o],
            recv_sem=x_recv.at[o],
            device_id={"tp": lax.rem(tp + o, ntp)},
            device_id_type=pl.DeviceIdType.MESH,
        )

    @pl.loop(1, ntp)
    def _(o):
        x_copy(o).start()

    def state_copy(o, msg, got, send, recv, flipped):
        peer = lax.rem(sp + o, nsp)
        ahead = (sp + o) // nsp
        which = 1 - ahead if flipped else ahead
        return pltpu.make_async_remote_copy(
            src_ref=msg.at[which],
            dst_ref=got.at[o],
            send_sem=send.at[o],
            recv_sem=recv.at[o],
            device_id={"sp": peer},
            device_id_type=pl.DeviceIdType.MESH,
        )

    def first_copy(o):
        return state_copy(o, msg1, got1, a_send, a_recv, False)

    def second_copy(o):
        return state_copy(o, msg2, got2, b_send, b_recv, True)

    def term_copy(o):
        peer = lax.rem(sp + o, nsp)
        return pltpu.make_async_remote_copy(
            src_ref=part.at[pl.ds(pl.multiple_of(peer * rows, rows), rows)],
            dst_ref=terms.at[o],
            send_sem=c_send.at[o],
            recv_sem=c_recv.at[o],
            device_id={"sp": peer},
            device_id_type=pl.DeviceIdType.MESH,
        )

    row = lax.broadcasted_iota(jnp.int32, (length, length), 0)
    col = lax.broadcasted_iota(jnp.int32, (length, length), 1)
    masks = (row >= col, row <= col)
    tris = tuple(jnp.where(m, 1.0, 0.0).astype(BF16) for m in masks)
    strict = (
        jnp.where(row > col, 1.0, 0.0).astype(BF16),
        jnp.where(row < col, 1.0, 0.0).astype(BF16),
    )
    ends = (length - 1, 0)
    mids = (half - 1, half)
    gates = (f_ref, r_ref)

    def head(a, h):
        return a[:, h * WIDTH : (h + 1) * WIDTH]

    def keys_of(j):
        sig = sigmoid(-gates[j][...].astype(F32))
        return sig, slack_ref[j : j + 1, :] * sig

    values = v_ref[...]

    for j in range(2):
        _, keys = keys_of(j)
        spikes = jnp.concatenate(
            [jnp.broadcast_to(decay_ref[j, :, h : h + 1], (length, WIDTH)) for h in range(heads)], axis=1
        )
        running = split_dot(tris[j], jnp.log(1.0 - keys) + spikes)
        run_s[j] = running
        closing = running[ends[j] : ends[j] + 1]
        key_end = (keys * jnp.exp(closing - running)).astype(BF16)
        shrink = jnp.exp(closing)
        hi = shrink.astype(BF16).astype(F32)
        lo = shrink - hi
        place = lax.broadcasted_iota(jnp.int32, (EXTRA, WIDTH), 0)
        for h in range(heads):
            base = h * (WIDTH + EXTRA)
            msg1[j, base : base + WIDTH] = tn(head(values, h), head(key_end, h)).astype(BF16)
            tail = jnp.where(place == 0, head(hi, h), jnp.where(place == 1, head(lo, h), 0.0)).astype(BF16)
            msg1[j, base + WIDTH : base + WIDTH + EXTRA] = tail
            msg2[j, base + WIDTH : base + WIDTH + EXTRA] = tail

    @pl.loop(1, nsp)
    def _(o):
        first_copy(o).start()

    total = None
    own_w.wait()
    own_x.wait()
    for o in range(ntp):
        if o > 0:
            x_copy(o).wait_recv()
        owner = lax.rem(tp - o + ntp, ntp)
        term = nn(xg[o], wv[pl.ds(pl.multiple_of(owner * feat, feat), feat), :])
        total = term if total is None else total + term
    pre = total.astype(BF16).astype(F32)
    sig_q = sigmoid(pre)
    queries = pre * sig_q * WIDTH**-0.5
    slope = sig_q * (1.0 + pre * (1.0 - sig_q)) * WIDTH**-0.5

    def gather_states(copy_of, got, near, far):
        acc[...] = jnp.zeros_like(acc)
        ones = jnp.ones((heads, 1, WIDTH), F32)

        def one(o, weights):
            copy_of(o).wait_recv()
            new = []
            for h in range(heads):
                base = h * (WIDTH + EXTRA)
                tail = got[o, base + WIDTH : base + WIDTH + EXTRA].astype(F32)
                shrink = tail[0:1] + tail[1:2]
                lanes = slice(h * WIDTH, (h + 1) * WIDTH)
                state = got[o, base : base + WIDTH].astype(F32)

                @pl.when(o <= sp)
                def _():
                    acc[near, :, lanes] += weights[h] * state

                @pl.when(o > sp)
                def _():
                    acc[far, :, lanes] = shrink * acc[far, :, lanes] + state

                new.append(weights[h] * shrink)
            return tuple(new)

        lax.fori_loop(1, nsp, one, tuple(ones[h] for h in range(heads)))

    gather_states(first_copy, got1, 0, 1)
    entry = (acc[0], acc[1])
    entry_bf = tuple(e.astype(BF16) for e in entry)

    q_dec, k_dec, k_low, q_in = [], [], [], []
    for j in range(2):
        running = run_s[j]
        _, keys = keys_of(j)
        middle = running[mids[j] : mids[j] + 1]
        q_dec.append((queries * jnp.exp(running - middle)).astype(BF16))
        hi, lo = split(keys * jnp.exp(middle - running))
        k_dec.append(hi)
        k_low.append(lo)
        q_in.append((queries * jnp.exp(running)).astype(BF16))

    cot = cot_ref[...].astype(F32) * gain_ref[...]
    for h in range(heads):
        lanes = slice(h * WIDTH, (h + 1) * WIDTH)
        value = head(values, h)
        scores = None
        mixed = None
        for j in range(2):
            s = nt(head(q_dec[j], h), head(k_dec[j], h)) + nt(head(q_dec[j], h), head(k_low[j], h))
            s = jnp.where(masks[j], s, 0.0)
            scores = s if scores is None else scores + s
            m = nt(head(q_in[j], h), head(entry_bf[j], h))
            mixed = m if mixed is None else mixed + m
        scores, scores_low = split(scores)
        mixed = mixed + (nn(scores, value) + nn(scores_low, value))
        scale = lax.rsqrt(jnp.mean(mixed * mixed, axis=-1, keepdims=True) + EPSILON)
        normed = mixed * scale
        grad = cot[:, lanes]
        d_out = scale * (grad - normed * jnp.mean(grad * normed, axis=-1, keepdims=True))
        d_out, d_low = split(d_out)
        d_scores = nt(d_out, value) + nt(d_low, value)
        dq_total = jnp.zeros((length, WIDTH), F32)
        for j in range(2):
            base = h * (WIDTH + EXTRA)
            msg2[j, base : base + WIDTH] = tn(d_out, head(q_in[j], h)).astype(BF16)
            ds, ds_low = split(jnp.where(masks[j], d_scores, 0.0))
            dq_loc = nn(ds, head(k_dec[j], h))
            dk_loc = tn(ds, head(q_dec[j], h))
            dq_low = nn(ds_low, head(k_dec[j], h)) + nn(ds, head(k_low[j], h))
            dq_far = nn(d_out, head(entry_bf[j], h)) + nn(d_low, head(entry_bf[j], h))
            running = run_s[j, :, lanes]
            middle = running[mids[j] : mids[j] + 1]
            dq_total = dq_total + (dq_loc + dq_low) * jnp.exp(running - middle) + dq_far * jnp.exp(running)
            qd = head(q_dec[j], h).astype(F32)
            kd = head(k_dec[j], h).astype(F32)
            loc_s[j, :, lanes] = qd * dq_loc - kd * dk_loc + head(q_in[j], h).astype(F32) * dq_far
            dk_s[j, :, lanes] = dk_loc * jnp.exp(middle - running)
        dqs_s[:, lanes] = tn(scores, d_out)
        dq_ref[:, lanes] = (dq_total * slope[:, lanes]).astype(BF16)

    @pl.loop(1, nsp)
    def _(o):
        second_copy(o).start()

    dq = dq_ref[...]
    for o in range(ntp):
        owner = lax.rem(tp - o + ntp, ntp)
        part[pl.ds(pl.multiple_of(owner * feat, feat), feat), :] = tn(xg[o], dq).astype(BF16)

    @pl.loop(1, nsp)
    def _(o):
        term_copy(o).start()

    gather_states(second_copy, got2, 1, 0)
    dv = dqs_s[...]
    outs = (gf_ref, gb_ref)
    for j in range(2):
        leave = acc[j]
        leave_bf = leave.astype(BF16)
        running = run_s[j]
        closing = running[ends[j] : ends[j] + 1]
        sig, keys = keys_of(j)
        end_scale = jnp.exp(closing - running)
        key_end = keys * end_scale
        key_end_bf = key_end.astype(BF16)
        dk_far = jnp.concatenate([nn(head(values, h), head(leave_bf, h)) for h in range(heads)], axis=1)
        dv = dv + jnp.concatenate([nt(head(key_end_bf, h), head(leave_bf, h)) for h in range(heads)], axis=1)
        dk = dk_s[j] + end_scale * dk_far
        through = jnp.exp(closing) * jnp.sum(entry[j] * leave, axis=0, keepdims=True)
        d_log = split_dot(tris[1 - j], loc_s[j]) + split_dot(strict[j], key_end * dk_far) + through
        outs[j][...] = slack_ref[j : j + 1, :] * sig * (1.0 - sig) * (d_log / (1.0 - keys) - dk)
    dv_ref[...] = dv.astype(BF16)

    wg_ref[...] = part[pl.ds(pl.multiple_of(sp * rows, rows), rows), :].astype(F32)

    @pl.loop(1, nsp)
    def _(o):
        term_copy(o).wait_recv()
        wg_ref[...] += terms[o].astype(F32)

    @pl.loop(1, ntp)
    def _(o):
        x_copy(o).wait_send()

    @pl.loop(1, nsp)
    def _(o):
        first_copy(o).wait_send()
        second_copy(o).wait_send()
        term_copy(o).wait_send()


def on_device(nsp, ntp, x, w, v, f, r, slack, decay, gain, cot):
    length, width = v.shape
    heads = width // WIDTH
    feat = x.shape[1]
    depth = w.shape[0]
    rows = depth // nsp
    message = (heads * (WIDTH + EXTRA), WIDTH)
    vmem = pl.BlockSpec(memory_space=pltpu.VMEM)
    anywhere = pl.BlockSpec(memory_space=pl.ANY)
    shape = jax.ShapeDtypeStruct
    dma = pltpu.SemaphoreType.DMA
    return pl.pallas_call(
        functools.partial(kernel, nsp, ntp),
        out_shape=(
            shape((length, width), BF16),
            shape((length, width), F32),
            shape((length, width), F32),
            shape((length, width), BF16),
            shape((rows, width), F32),
        ),
        in_specs=[anywhere, anywhere] + [vmem] * 7,
        out_specs=(vmem,) * 5,
        scratch_shapes=[
            pltpu.VMEM((ntp, length, feat), BF16),
            pltpu.VMEM((depth, width), BF16),
            pltpu.VMEM((2,) + message, BF16),
            pltpu.VMEM((nsp,) + message, BF16),
            pltpu.VMEM((2,) + message, BF16),
            pltpu.VMEM((nsp,) + message, BF16),
            pltpu.VMEM((2, WIDTH, width), F32),
            pltpu.VMEM((depth, width), BF16),
            pltpu.VMEM((nsp, rows, width), BF16),
            pltpu.VMEM((2, length, width), F32),
            pltpu.VMEM((length, width), F32),
            pltpu.VMEM((2, length, width), F32),
            pltpu.VMEM((2, length, width), F32),
            dma((2,)),
            dma((ntp,)),
            dma((ntp,)),
            dma((nsp,)),
            dma((nsp,)),
            dma((nsp,)),
            dma((nsp,)),
            dma((nsp,)),
            dma((nsp,)),
        ],
        compiler_params=pltpu.CompilerParams(
            collective_id=0, has_side_effects=True, vmem_limit_bytes=50 * 1024 * 1024
        ),
    )(x, w, v, f, r, slack, decay, gain.reshape(1, width), cot)


def solution(mesh):
    placed = (
        P("sp", "tp"),
        P(None, "tp"),
        P("sp", "tp"),
        P("sp", "tp"),
        P("sp", "tp"),
        P(None, "tp"),
        P(None, "sp", "tp"),
        P("tp"),
        P("sp", "tp"),
    )
    return jax.shard_map(
        functools.partial(on_device, mesh.shape["sp"], mesh.shape["tp"]),
        mesh=mesh,
        in_specs=placed,
        out_specs=(P("sp", "tp"),) * 5,
        check_vma=False,
    )
```

```python
import functools

import jax
import jax.numpy as jnp
from jax import lax
from jax.experimental import pallas as pl
from jax.experimental.pallas import tpu as pltpu
from jax.sharding import PartitionSpec as P

WIDTH = 128
EXTRA = 16
EPSILON = 1e-06
F32 = jnp.float32
BF16 = jnp.bfloat16


def dot(a, b, ca, cb):
    return lax.dot_general(a, b, (((ca,), (cb,)), ((), ())), preferred_element_type=F32)


def nn(a, b):
    return dot(a, b, 1, 0)


def nt(a, b):
    return dot(a, b, 1, 1)


def tn(a, b):
    return dot(a, b, 0, 0)


def split(a):
    hi = a.astype(BF16)
    return hi, (a - hi.astype(F32)).astype(BF16)


def split_dot(tri, a):
    hi, lo = split(a)
    return nn(tri, hi) + nn(tri, lo)


def sigmoid(x):
    return 1.0 / (1.0 + jnp.exp(-x))


def kernel(
    nsp,
    ntp,
    x_hbm,
    w_hbm,
    v_hbm,
    f_hbm,
    r_hbm,
    slack_hbm,
    decay_hbm,
    gain_hbm,
    cot_hbm,
    dq_ref,
    gf_ref,
    gb_ref,
    dv_ref,
    wg_ref,
    v_ref,
    f_ref,
    r_ref,
    slack_ref,
    decay_ref,
    gain_ref,
    cot_ref,
    xg,
    wv,
    msg1,
    got1,
    msg2,
    got2,
    acc,
    part,
    terms,
    run_s,
    dqs_s,
    loc_s,
    dk_s,
    local_sem,
    x_send,
    x_recv,
    a_send,
    a_recv,
    b_send,
    b_recv,
    c_send,
    c_recv,
):
    sp = lax.axis_index("sp")
    tp = lax.axis_index("tp")
    length, width = v_hbm.shape
    heads = width // WIDTH
    feat = x_hbm.shape[1]
    rows = wg_ref.shape[0]
    half = length // 2

    own_x = pltpu.make_async_copy(x_hbm, xg.at[tp], local_sem.at[0])
    own_w = pltpu.make_async_copy(w_hbm, wv, local_sem.at[1])
    small = [
        pltpu.make_async_copy(source, target, local_sem.at[2 + i])
        for i, (source, target) in enumerate(
            (
                (f_hbm, f_ref),
                (r_hbm, r_ref),
                (decay_hbm, decay_ref),
                (slack_hbm, slack_ref),
                (v_hbm, v_ref),
                (gain_hbm, gain_ref),
                (cot_hbm, cot_ref),
            )
        )
    ]
    for copy in small:
        copy.start()
    own_x.start()
    own_w.start()

    barrier = pltpu.get_barrier_semaphore()

    @pl.loop(1, ntp)
    def _(o):
        pl.semaphore_signal(
            barrier, inc=1, device_id={"tp": lax.rem(tp + o, ntp)}, device_id_type=pl.DeviceIdType.MESH
        )

    @pl.loop(1, nsp)
    def _(o):
        pl.semaphore_signal(
            barrier, inc=1, device_id={"sp": lax.rem(sp + o, nsp)}, device_id_type=pl.DeviceIdType.MESH
        )

    pl.semaphore_wait(barrier, nsp + ntp - 2)

    chips = ntp // 2
    chip, core = tp // 2, lax.rem(tp, 2)
    sibling = chip * 2 + 1 - core

    def x_copy(source, owner, place, target):
        return pltpu.make_async_remote_copy(
            src_ref=source,
            dst_ref=xg.at[owner],
            send_sem=x_send.at[place],
            recv_sem=x_recv.at[owner],
            device_id={"tp": target},
            device_id_type=pl.DeviceIdType.MESH,
        )

    direct = [
        x_copy(x_hbm, tp, i, lax.rem(chip + i, chips) * 2 + core) for i in range(1, chips)
    ] + [x_copy(x_hbm, tp, 0, sibling)]
    for copy in direct:
        copy.start()

    def state_copy(o, msg, got, send, recv, flipped):
        peer = lax.rem(sp + o, nsp)
        ahead = (sp + o) // nsp
        which = 1 - ahead if flipped else ahead
        return pltpu.make_async_remote_copy(
            src_ref=msg.at[which],
            dst_ref=got.at[o],
            send_sem=send.at[o],
            recv_sem=recv.at[o],
            device_id={"sp": peer},
            device_id_type=pl.DeviceIdType.MESH,
        )

    def first_copy(o):
        return state_copy(o, msg1, got1, a_send, a_recv, False)

    def second_copy(o):
        return state_copy(o, msg2, got2, b_send, b_recv, True)

    def term_copy(o):
        peer = lax.rem(sp + o, nsp)
        return pltpu.make_async_remote_copy(
            src_ref=part.at[pl.ds(pl.multiple_of(peer * rows, rows), rows)],
            dst_ref=terms.at[o],
            send_sem=c_send.at[o],
            recv_sem=c_recv.at[o],
            device_id={"sp": peer},
            device_id_type=pl.DeviceIdType.MESH,
        )

    row = lax.broadcasted_iota(jnp.int32, (length, length), 0)
    col = lax.broadcasted_iota(jnp.int32, (length, length), 1)
    masks = (row >= col, row <= col)
    tris = tuple(jnp.where(m, 1.0, 0.0).astype(BF16) for m in masks)
    strict = (
        jnp.where(row > col, 1.0, 0.0).astype(BF16),
        jnp.where(row < col, 1.0, 0.0).astype(BF16),
    )
    ends = (length - 1, 0)
    mids = (half - 1, half)
    gates = (f_ref, r_ref)

    def head(a, h):
        return a[:, h * WIDTH : (h + 1) * WIDTH]

    def keys_of(j):
        sig = sigmoid(-gates[j][...].astype(F32))
        return sig, slack_ref[j : j + 1, :] * sig

    for copy in small:
        copy.wait()
    values = v_ref[...]

    for j in range(2):
        _, keys = keys_of(j)
        spikes = jnp.concatenate(
            [jnp.broadcast_to(decay_ref[j, :, h : h + 1], (length, WIDTH)) for h in range(heads)], axis=1
        )
        running = split_dot(tris[j], jnp.log(1.0 - keys) + spikes)
        run_s[j] = running
        closing = running[ends[j] : ends[j] + 1]
        key_end = (keys * jnp.exp(closing - running)).astype(BF16)
        shrink = jnp.exp(closing)
        hi = shrink.astype(BF16).astype(F32)
        lo = shrink - hi
        place = lax.broadcasted_iota(jnp.int32, (EXTRA, WIDTH), 0)
        for h in range(heads):
            base = h * (WIDTH + EXTRA)
            msg1[j, base : base + WIDTH] = tn(head(values, h), head(key_end, h)).astype(BF16)
            tail = jnp.where(place == 0, head(hi, h), jnp.where(place == 1, head(lo, h), 0.0)).astype(BF16)
            msg1[j, base + WIDTH : base + WIDTH + EXTRA] = tail
            msg2[j, base + WIDTH : base + WIDTH + EXTRA] = tail

    @pl.loop(1, nsp)
    def _(o):
        first_copy(o).start()

    def project(owner):
        return nn(xg[owner], wv[pl.ds(pl.multiple_of(owner * feat, feat), feat), :])

    own_w.wait()
    own_x.wait()
    total = project(tp)
    x_copy(x_hbm, sibling, 0, sibling).wait_recv()
    total = total + project(sibling)
    passed = []
    for i in range(1, chips):
        owner = lax.rem(chip - i + chips, chips) * 2 + core
        x_copy(x_hbm, owner, 0, sibling).wait_recv()
        onward = x_copy(xg.at[owner], owner, chips + i, sibling)
        onward.start()
        passed.append(onward)
        total = total + project(owner)
        other = lax.rem(chip - i + chips, chips) * 2 + 1 - core
        x_copy(x_hbm, other, 0, sibling).wait_recv()
        total = total + project(other)
    pre = total.astype(BF16).astype(F32)
    sig_q = sigmoid(pre)
    queries = pre * sig_q * WIDTH**-0.5
    slope = sig_q * (1.0 + pre * (1.0 - sig_q)) * WIDTH**-0.5

    def gather_states(copy_of, got, near, far):
        acc[...] = jnp.zeros_like(acc)
        ones = jnp.ones((heads, 1, WIDTH), F32)

        def one(o, weights):
            copy_of(o).wait_recv()
            new = []
            for h in range(heads):
                base = h * (WIDTH + EXTRA)
                tail = got[o, base + WIDTH : base + WIDTH + EXTRA].astype(F32)
                shrink = tail[0:1] + tail[1:2]
                lanes = slice(h * WIDTH, (h + 1) * WIDTH)
                state = got[o, base : base + WIDTH].astype(F32)

                @pl.when(o <= sp)
                def _():
                    acc[near, :, lanes] += weights[h] * state

                @pl.when(o > sp)
                def _():
                    acc[far, :, lanes] = shrink * acc[far, :, lanes] + state

                new.append(weights[h] * shrink)
            return tuple(new)

        lax.fori_loop(1, nsp, one, tuple(ones[h] for h in range(heads)))

    gather_states(first_copy, got1, 0, 1)
    entry = (acc[0], acc[1])
    entry_bf = tuple(e.astype(BF16) for e in entry)

    q_dec, k_dec, k_low, q_in = [], [], [], []
    for j in range(2):
        running = run_s[j]
        _, keys = keys_of(j)
        middle = running[mids[j] : mids[j] + 1]
        q_dec.append((queries * jnp.exp(running - middle)).astype(BF16))
        hi, lo = split(keys * jnp.exp(middle - running))
        k_dec.append(hi)
        k_low.append(lo)
        q_in.append((queries * jnp.exp(running)).astype(BF16))

    cot = cot_ref[...].astype(F32) * gain_ref[...]
    for h in range(heads):
        lanes = slice(h * WIDTH, (h + 1) * WIDTH)
        value = head(values, h)
        scores = None
        mixed = None
        for j in range(2):
            s = nt(head(q_dec[j], h), head(k_dec[j], h)) + nt(head(q_dec[j], h), head(k_low[j], h))
            s = jnp.where(masks[j], s, 0.0)
            scores = s if scores is None else scores + s
            m = nt(head(q_in[j], h), head(entry_bf[j], h))
            mixed = m if mixed is None else mixed + m
        scores, scores_low = split(scores)
        mixed = mixed + (nn(scores, value) + nn(scores_low, value))
        scale = lax.rsqrt(jnp.mean(mixed * mixed, axis=-1, keepdims=True) + EPSILON)
        normed = mixed * scale
        grad = cot[:, lanes]
        d_out = scale * (grad - normed * jnp.mean(grad * normed, axis=-1, keepdims=True))
        d_out, d_low = split(d_out)
        d_scores = nt(d_out, value) + nt(d_low, value)
        dq_total = jnp.zeros((length, WIDTH), F32)
        for j in range(2):
            base = h * (WIDTH + EXTRA)
            msg2[j, base : base + WIDTH] = tn(d_out, head(q_in[j], h)).astype(BF16)
            ds, ds_low = split(jnp.where(masks[j], d_scores, 0.0))
            dq_loc = nn(ds, head(k_dec[j], h))
            dk_loc = tn(ds, head(q_dec[j], h))
            dq_low = nn(ds_low, head(k_dec[j], h)) + nn(ds, head(k_low[j], h))
            dq_far = nn(d_out, head(entry_bf[j], h)) + nn(d_low, head(entry_bf[j], h))
            running = run_s[j, :, lanes]
            middle = running[mids[j] : mids[j] + 1]
            dq_total = dq_total + (dq_loc + dq_low) * jnp.exp(running - middle) + dq_far * jnp.exp(running)
            qd = head(q_dec[j], h).astype(F32)
            kd = head(k_dec[j], h).astype(F32)
            loc_s[j, :, lanes] = qd * dq_loc - kd * dk_loc + head(q_in[j], h).astype(F32) * dq_far
            dk_s[j, :, lanes] = dk_loc * jnp.exp(middle - running)
        dqs_s[:, lanes] = tn(scores, d_out)
        dq_ref[:, lanes] = (dq_total * slope[:, lanes]).astype(BF16)

    @pl.loop(1, nsp)
    def _(o):
        second_copy(o).start()

    dq = dq_ref[...]
    for o in range(ntp):
        part[o * feat : (o + 1) * feat, :] = tn(xg[o], dq).astype(BF16)

    @pl.loop(1, nsp)
    def _(o):
        term_copy(o).start()

    gather_states(second_copy, got2, 1, 0)
    dv = dqs_s[...]
    outs = (gf_ref, gb_ref)
    for j in range(2):
        leave = acc[j]
        leave_bf = leave.astype(BF16)
        running = run_s[j]
        closing = running[ends[j] : ends[j] + 1]
        sig, keys = keys_of(j)
        end_scale = jnp.exp(closing - running)
        key_end = keys * end_scale
        key_end_bf = key_end.astype(BF16)
        dk_far = jnp.concatenate([nn(head(values, h), head(leave_bf, h)) for h in range(heads)], axis=1)
        dv = dv + jnp.concatenate([nt(head(key_end_bf, h), head(leave_bf, h)) for h in range(heads)], axis=1)
        dk = dk_s[j] + end_scale * dk_far
        through = jnp.exp(closing) * jnp.sum(entry[j] * leave, axis=0, keepdims=True)
        d_log = split_dot(tris[1 - j], loc_s[j]) + split_dot(strict[j], key_end * dk_far) + through
        outs[j][...] = slack_ref[j : j + 1, :] * sig * (1.0 - sig) * (d_log / (1.0 - keys) - dk)
    dv_ref[...] = dv.astype(BF16)

    wg_ref[...] = part[pl.ds(pl.multiple_of(sp * rows, rows), rows), :].astype(F32)

    @pl.loop(1, nsp)
    def _(o):
        term_copy(o).wait_recv()
        wg_ref[...] += terms[o].astype(F32)

    for copy in direct + passed:
        copy.wait_send()

    @pl.loop(1, nsp)
    def _(o):
        first_copy(o).wait_send()
        second_copy(o).wait_send()
        term_copy(o).wait_send()


def on_device(nsp, ntp, x, w, v, f, r, slack, decay, gain, cot):
    length, width = v.shape
    heads = width // WIDTH
    feat = x.shape[1]
    depth = w.shape[0]
    rows = depth // nsp
    message = (heads * (WIDTH + EXTRA), WIDTH)
    vmem = pl.BlockSpec(memory_space=pltpu.VMEM)
    anywhere = pl.BlockSpec(memory_space=pltpu.HBM)
    shape = jax.ShapeDtypeStruct
    dma = pltpu.SemaphoreType.DMA
    return pl.pallas_call(
        functools.partial(kernel, nsp, ntp),
        out_shape=(
            shape((length, width), BF16),
            shape((length, width), F32),
            shape((length, width), F32),
            shape((length, width), BF16),
            shape((rows, width), F32),
        ),
        in_specs=[anywhere] * 9,
        out_specs=(vmem,) * 5,
        scratch_shapes=[
            pltpu.VMEM((length, width), BF16),
            pltpu.VMEM((length, width), BF16),
            pltpu.VMEM((length, width), BF16),
            pltpu.VMEM((2, width), F32),
            pltpu.VMEM((2, length, heads), F32),
            pltpu.VMEM((1, width), F32),
            pltpu.VMEM((length, width), BF16),
            pltpu.VMEM((ntp, length, feat), BF16),
            pltpu.VMEM((depth, width), BF16),
            pltpu.VMEM((2,) + message, BF16),
            pltpu.VMEM((nsp,) + message, BF16),
            pltpu.VMEM((2,) + message, BF16),
            pltpu.VMEM((nsp,) + message, BF16),
            pltpu.VMEM((2, WIDTH, width), F32),
            pltpu.VMEM((depth, width), BF16),
            pltpu.VMEM((nsp, rows, width), BF16),
            pltpu.VMEM((2, length, width), F32),
            pltpu.VMEM((length, width), F32),
            pltpu.VMEM((2, length, width), F32),
            pltpu.VMEM((2, length, width), F32),
            dma((9,)),
            dma((ntp,)),
            dma((ntp,)),
            dma((nsp,)),
            dma((nsp,)),
            dma((nsp,)),
            dma((nsp,)),
            dma((nsp,)),
            dma((nsp,)),
        ],
        compiler_params=pltpu.CompilerParams(
            collective_id=0, has_side_effects=True, vmem_limit_bytes=50 * 1024 * 1024
        ),
    )(x, w, v, f, r, slack, decay, gain.reshape(1, width), cot)


def solution(mesh):
    placed = (
        P("sp", "tp"),
        P(None, "tp"),
        P("sp", "tp"),
        P("sp", "tp"),
        P("sp", "tp"),
        P(None, "tp"),
        P(None, "sp", "tp"),
        P("tp"),
        P("sp", "tp"),
    )
    return jax.shard_map(
        functools.partial(on_device, mesh.shape["sp"], mesh.shape["tp"]),
        mesh=mesh,
        in_specs=placed,
        out_specs=(P("sp", "tp"),) * 5,
        check_vma=False,
    )
```

```python
import functools

import jax
import jax.numpy as jnp
from jax import lax
from jax.experimental import pallas as pl
from jax.experimental.pallas import tpu as pltpu
from jax.sharding import PartitionSpec as P

WIDTH = 128
EXTRA = 16
EPSILON = 1e-06
F32 = jnp.float32
BF16 = jnp.bfloat16


def dot(a, b, ca, cb):
    return lax.dot_general(a, b, (((ca,), (cb,)), ((), ())), preferred_element_type=F32)


def nn(a, b):
    return dot(a, b, 1, 0)


def nt(a, b):
    return dot(a, b, 1, 1)


def tn(a, b):
    return dot(a, b, 0, 0)


def split(a):
    hi = a.astype(BF16)
    return hi, (a - hi.astype(F32)).astype(BF16)


def split_dot(tri, a):
    hi, lo = split(a)
    return nn(tri, hi) + nn(tri, lo)


def sigmoid(x):
    return 1.0 / (1.0 + jnp.exp(-x))


def kernel(
    nsp,
    ntp,
    x_hbm,
    w_hbm,
    v_hbm,
    f_hbm,
    r_hbm,
    slack_hbm,
    decay_hbm,
    gain_hbm,
    cot_hbm,
    dq_ref,
    gf_ref,
    gb_ref,
    dv_ref,
    wg_ref,
    v_ref,
    f_ref,
    r_ref,
    slack_ref,
    decay_ref,
    gain_ref,
    cot_ref,
    xg,
    wv,
    msg1,
    got1,
    msg2,
    got2,
    acc,
    part,
    terms,
    run_s,
    dqs_s,
    loc_s,
    dk_s,
    local_sem,
    x_send,
    x_recv,
    a_send,
    a_recv,
    b_send,
    b_recv,
    c_send,
    c_recv,
):
    sp = lax.axis_index("sp")
    tp = lax.axis_index("tp")
    length, width = v_hbm.shape
    heads = width // WIDTH
    feat = x_hbm.shape[1]
    rows = wg_ref.shape[0]
    half = length // 2

    own_x = pltpu.make_async_copy(x_hbm, xg.at[tp], local_sem.at[0])
    own_w = pltpu.make_async_copy(w_hbm, wv, local_sem.at[1])
    small = [
        pltpu.make_async_copy(source, target, local_sem.at[2 + i])
        for i, (source, target) in enumerate(
            (
                (f_hbm, f_ref),
                (r_hbm, r_ref),
                (decay_hbm, decay_ref),
                (slack_hbm, slack_ref),
                (v_hbm, v_ref),
                (gain_hbm, gain_ref),
                (cot_hbm, cot_ref),
            )
        )
    ]
    for copy in small:
        copy.start()
    own_x.start()
    own_w.start()

    barrier = pltpu.get_barrier_semaphore()

    @pl.loop(1, ntp)
    def _(o):
        pl.semaphore_signal(
            barrier, inc=1, device_id={"tp": lax.rem(tp + o, ntp)}, device_id_type=pl.DeviceIdType.MESH
        )

    @pl.loop(1, nsp)
    def _(o):
        pl.semaphore_signal(
            barrier, inc=1, device_id={"sp": lax.rem(sp + o, nsp)}, device_id_type=pl.DeviceIdType.MESH
        )

    pl.semaphore_wait(barrier, nsp + ntp - 2)

    chips = ntp // 2
    chip, core = tp // 2, lax.rem(tp, 2)
    sibling = chip * 2 + 1 - core

    def x_copy(source, owner, place, target):
        return pltpu.make_async_remote_copy(
            src_ref=source,
            dst_ref=xg.at[owner],
            send_sem=x_send.at[place],
            recv_sem=x_recv.at[owner],
            device_id={"tp": target},
            device_id_type=pl.DeviceIdType.MESH,
        )

    direct = [
        x_copy(x_hbm, tp, i, lax.rem(chip + i, chips) * 2 + core) for i in range(1, chips)
    ] + [x_copy(x_hbm, tp, 0, sibling)]
    for copy in direct:
        copy.start()

    def state_copy(o, msg, got, send, recv, flipped):
        peer = lax.rem(sp + o, nsp)
        ahead = (sp + o) // nsp
        which = 1 - ahead if flipped else ahead
        return pltpu.make_async_remote_copy(
            src_ref=msg.at[which],
            dst_ref=got.at[o],
            send_sem=send.at[o],
            recv_sem=recv.at[o],
            device_id={"sp": peer},
            device_id_type=pl.DeviceIdType.MESH,
        )

    def first_copy(o):
        return state_copy(o, msg1, got1, a_send, a_recv, False)

    def second_copy(o):
        return state_copy(o, msg2, got2, b_send, b_recv, True)

    def term_copy(o):
        peer = lax.rem(sp + o, nsp)
        return pltpu.make_async_remote_copy(
            src_ref=part.at[pl.ds(pl.multiple_of(peer * rows, rows), rows)],
            dst_ref=terms.at[o],
            send_sem=c_send.at[o],
            recv_sem=c_recv.at[o],
            device_id={"sp": peer},
            device_id_type=pl.DeviceIdType.MESH,
        )

    row = lax.broadcasted_iota(jnp.int32, (length, length), 0)
    col = lax.broadcasted_iota(jnp.int32, (length, length), 1)
    masks = (row >= col, row <= col)
    tris = tuple(jnp.where(m, 1.0, 0.0).astype(BF16) for m in masks)
    strict = (
        jnp.where(row > col, 1.0, 0.0).astype(BF16),
        jnp.where(row < col, 1.0, 0.0).astype(BF16),
    )
    ends = (length - 1, 0)
    mids = (half - 1, half)
    gates = (f_ref, r_ref)

    def head(a, h):
        return a[:, h * WIDTH : (h + 1) * WIDTH]

    def keys_of(j):
        sig = sigmoid(-gates[j][...].astype(F32))
        return sig, slack_ref[j : j + 1, :] * sig

    for copy in small:
        copy.wait()
    values = v_ref[...]

    for j in range(2):
        _, keys = keys_of(j)
        spikes = jnp.concatenate(
            [jnp.broadcast_to(decay_ref[j, :, h : h + 1], (length, WIDTH)) for h in range(heads)], axis=1
        )
        running = split_dot(tris[j], jnp.log(1.0 - keys) + spikes)
        run_s[j] = running
        closing = running[ends[j] : ends[j] + 1]
        key_end = (keys * jnp.exp(closing - running)).astype(BF16)
        shrink = jnp.exp(closing)
        hi = shrink.astype(BF16).astype(F32)
        lo = shrink - hi
        place = lax.broadcasted_iota(jnp.int32, (EXTRA, WIDTH), 0)
        for h in range(heads):
            base = h * (WIDTH + EXTRA)
            msg1[j, base : base + WIDTH] = tn(head(values, h), head(key_end, h)).astype(BF16)
            tail = jnp.where(place == 0, head(hi, h), jnp.where(place == 1, head(lo, h), 0.0)).astype(BF16)
            msg1[j, base + WIDTH : base + WIDTH + EXTRA] = tail
            msg2[j, base + WIDTH : base + WIDTH + EXTRA] = tail

    @pl.loop(1, nsp)
    def _(o):
        first_copy(o).start()

    def project(owner):
        return nn(xg[owner], wv[pl.ds(pl.multiple_of(owner * feat, feat), feat), :])

    own_w.wait()
    own_x.wait()
    total = project(tp)
    x_copy(x_hbm, sibling, 0, sibling).wait_recv()
    total = total + project(sibling)
    passed = []
    for i in range(1, chips):
        owner = lax.rem(chip - i + chips, chips) * 2 + core
        x_copy(x_hbm, owner, 0, sibling).wait_recv()
        onward = x_copy(xg.at[owner], owner, chips + i, sibling)
        onward.start()
        passed.append(onward)
        total = total + project(owner)
        other = lax.rem(chip - i + chips, chips) * 2 + 1 - core
        x_copy(x_hbm, other, 0, sibling).wait_recv()
        total = total + project(other)
    pre = total.astype(BF16).astype(F32)
    sig_q = sigmoid(pre)
    queries = pre * sig_q * WIDTH**-0.5
    slope = sig_q * (1.0 + pre * (1.0 - sig_q)) * WIDTH**-0.5

    def gather_states(copy_of, got, near, far):
        acc[...] = jnp.zeros_like(acc)
        ones = jnp.ones((heads, 1, WIDTH), F32)

        def one(o, weights):
            copy_of(o).wait_recv()
            new = []
            for h in range(heads):
                base = h * (WIDTH + EXTRA)
                tail = got[o, base + WIDTH : base + WIDTH + EXTRA].astype(F32)
                shrink = tail[0:1] + tail[1:2]
                lanes = slice(h * WIDTH, (h + 1) * WIDTH)
                state = got[o, base : base + WIDTH].astype(F32)

                @pl.when(o <= sp)
                def _():
                    acc[near, :, lanes] += weights[h] * state

                @pl.when(o > sp)
                def _():
                    acc[far, :, lanes] = shrink * acc[far, :, lanes] + state

                new.append(weights[h] * shrink)
            return tuple(new)

        lax.fori_loop(1, nsp, one, tuple(ones[h] for h in range(heads)))

    gather_states(first_copy, got1, 0, 1)
    entry = (acc[0], acc[1])
    entry_bf = tuple(e.astype(BF16) for e in entry)

    q_dec, k_dec, k_low, q_in = [], [], [], []
    for j in range(2):
        running = run_s[j]
        _, keys = keys_of(j)
        middle = running[mids[j] : mids[j] + 1]
        q_dec.append((queries * jnp.exp(running - middle)).astype(BF16))
        hi, lo = split(keys * jnp.exp(middle - running))
        k_dec.append(hi)
        k_low.append(lo)
        q_in.append((queries * jnp.exp(running)).astype(BF16))

    cot = cot_ref[...].astype(F32) * gain_ref[...]
    for h in range(heads):
        lanes = slice(h * WIDTH, (h + 1) * WIDTH)
        value = head(values, h)
        scores = None
        mixed = None
        for j in range(2):
            s = nt(head(q_dec[j], h), head(k_dec[j], h)) + nt(head(q_dec[j], h), head(k_low[j], h))
            s = jnp.where(masks[j], s, 0.0)
            scores = s if scores is None else scores + s
            m = nt(head(q_in[j], h), head(entry_bf[j], h))
            mixed = m if mixed is None else mixed + m
        scores, scores_low = split(scores)
        mixed = mixed + (nn(scores, value) + nn(scores_low, value))
        scale = lax.rsqrt(jnp.mean(mixed * mixed, axis=-1, keepdims=True) + EPSILON)
        normed = mixed * scale
        grad = cot[:, lanes]
        d_out = scale * (grad - normed * jnp.mean(grad * normed, axis=-1, keepdims=True))
        d_out, d_low = split(d_out)
        d_scores = nt(d_out, value) + nt(d_low, value)
        dq_total = jnp.zeros((length, WIDTH), F32)
        for j in range(2):
            base = h * (WIDTH + EXTRA)
            msg2[j, base : base + WIDTH] = tn(d_out, head(q_in[j], h)).astype(BF16)
            ds, ds_low = split(jnp.where(masks[j], d_scores, 0.0))
            dq_loc = nn(ds, head(k_dec[j], h))
            dk_loc = tn(ds, head(q_dec[j], h))
            dq_low = nn(ds_low, head(k_dec[j], h)) + nn(ds, head(k_low[j], h))
            dq_far = nn(d_out, head(entry_bf[j], h)) + nn(d_low, head(entry_bf[j], h))
            running = run_s[j, :, lanes]
            middle = running[mids[j] : mids[j] + 1]
            dq_total = dq_total + (dq_loc + dq_low) * jnp.exp(running - middle) + dq_far * jnp.exp(running)
            qd = head(q_dec[j], h).astype(F32)
            kd = head(k_dec[j], h).astype(F32)
            loc_s[j, :, lanes] = qd * dq_loc - kd * dk_loc + head(q_in[j], h).astype(F32) * dq_far
            dk_s[j, :, lanes] = dk_loc * jnp.exp(middle - running)
        dqs_s[:, lanes] = tn(scores, d_out)
        dq_ref[:, lanes] = (dq_total * slope[:, lanes]).astype(BF16)

    @pl.loop(1, nsp)
    def _(o):
        second_copy(o).start()

    dq = dq_ref[...]
    share = nsp // ntp
    for o in range(ntp):
        block = lax.rem(sp // share + 1 + o, ntp)
        part[pl.ds(pl.multiple_of(block * feat, feat), feat), :] = tn(xg[block], dq).astype(BF16)

        @pl.loop(0, share)
        def _(i):
            ahead = lax.rem(block * share + i - sp + nsp, nsp)

            @pl.when(ahead > 0)
            def _():
                term_copy(ahead).start()

    gather_states(second_copy, got2, 1, 0)
    dv = dqs_s[...]
    outs = (gf_ref, gb_ref)
    for j in range(2):
        leave = acc[j]
        leave_bf = leave.astype(BF16)
        running = run_s[j]
        closing = running[ends[j] : ends[j] + 1]
        sig, keys = keys_of(j)
        end_scale = jnp.exp(closing - running)
        key_end = keys * end_scale
        key_end_bf = key_end.astype(BF16)
        dk_far = jnp.concatenate([nn(head(values, h), head(leave_bf, h)) for h in range(heads)], axis=1)
        dv = dv + jnp.concatenate([nt(head(key_end_bf, h), head(leave_bf, h)) for h in range(heads)], axis=1)
        dk = dk_s[j] + end_scale * dk_far
        through = jnp.exp(closing) * jnp.sum(entry[j] * leave, axis=0, keepdims=True)
        d_log = split_dot(tris[1 - j], loc_s[j]) + split_dot(strict[j], key_end * dk_far) + through
        outs[j][...] = slack_ref[j : j + 1, :] * sig * (1.0 - sig) * (d_log / (1.0 - keys) - dk)
    dv_ref[...] = dv.astype(BF16)

    wg_ref[...] = part[pl.ds(pl.multiple_of(sp * rows, rows), rows), :].astype(F32)

    @pl.loop(1, nsp)
    def _(o):
        term_copy(o).wait_recv()
        wg_ref[...] += terms[o].astype(F32)

    for copy in direct + passed:
        copy.wait_send()

    @pl.loop(1, nsp)
    def _(o):
        first_copy(o).wait_send()
        second_copy(o).wait_send()
        term_copy(o).wait_send()


def on_device(nsp, ntp, x, w, v, f, r, slack, decay, gain, cot):
    length, width = v.shape
    heads = width // WIDTH
    feat = x.shape[1]
    depth = w.shape[0]
    rows = depth // nsp
    message = (heads * (WIDTH + EXTRA), WIDTH)
    vmem = pl.BlockSpec(memory_space=pltpu.VMEM)
    anywhere = pl.BlockSpec(memory_space=pltpu.HBM)
    shape = jax.ShapeDtypeStruct
    dma = pltpu.SemaphoreType.DMA
    return pl.pallas_call(
        functools.partial(kernel, nsp, ntp),
        out_shape=(
            shape((length, width), BF16),
            shape((length, width), F32),
            shape((length, width), F32),
            shape((length, width), BF16),
            shape((rows, width), F32),
        ),
        in_specs=[anywhere] * 9,
        out_specs=(vmem,) * 5,
        scratch_shapes=[
            pltpu.VMEM((length, width), BF16),
            pltpu.VMEM((length, width), BF16),
            pltpu.VMEM((length, width), BF16),
            pltpu.VMEM((2, width), F32),
            pltpu.VMEM((2, length, heads), F32),
            pltpu.VMEM((1, width), F32),
            pltpu.VMEM((length, width), BF16),
            pltpu.VMEM((ntp, length, feat), BF16),
            pltpu.VMEM((depth, width), BF16),
            pltpu.VMEM((2,) + message, BF16),
            pltpu.VMEM((nsp,) + message, BF16),
            pltpu.VMEM((2,) + message, BF16),
            pltpu.VMEM((nsp,) + message, BF16),
            pltpu.VMEM((2, WIDTH, width), F32),
            pltpu.VMEM((depth, width), BF16),
            pltpu.VMEM((nsp, rows, width), BF16),
            pltpu.VMEM((2, length, width), F32),
            pltpu.VMEM((length, width), F32),
            pltpu.VMEM((2, length, width), F32),
            pltpu.VMEM((2, length, width), F32),
            dma((9,)),
            dma((ntp,)),
            dma((ntp,)),
            dma((nsp,)),
            dma((nsp,)),
            dma((nsp,)),
            dma((nsp,)),
            dma((nsp,)),
            dma((nsp,)),
        ],
        compiler_params=pltpu.CompilerParams(
            collective_id=0, has_side_effects=True, vmem_limit_bytes=50 * 1024 * 1024
        ),
    )(x, w, v, f, r, slack, decay, gain.reshape(1, width), cot)


def solution(mesh):
    placed = (
        P("sp", "tp"),
        P(None, "tp"),
        P("sp", "tp"),
        P("sp", "tp"),
        P("sp", "tp"),
        P(None, "tp"),
        P(None, "sp", "tp"),
        P("tp"),
        P("sp", "tp"),
    )
    return jax.shard_map(
        functools.partial(on_device, mesh.shape["sp"], mesh.shape["tp"]),
        mesh=mesh,
        in_specs=placed,
        out_specs=(P("sp", "tp"),) * 5,
        check_vma=False,
    )
```
